32 devices in a mesh: sp: 16 (over z, y, x), tp: 2 (over core).
Axes of the slice: x: 2, y: 2, z: 4, core: 2. Of those that a mesh axis runs over, the one named last changes fastest.
Arguments:
- tokens: bfloat16 [8192, 4096], P('sp', 'tp'), may hold values from -6 to 6
- norm_gain: float32 [4096], replicated, may hold values from 0.1 to 1.9
- w_query: bfloat16 [4096, 2048], P('sp', 'tp'), may hold values from -0.09375 to 0.09375
- w_key: bfloat16 [4096, 512], P('sp', 'tp'), may hold values from -0.09375 to 0.09375
- w_value: bfloat16 [4096, 512], P('sp', 'tp'), may hold values from -0.09375 to 0.09375
- w_pool_in: bfloat16 [4096, 2048], P('sp', 'tp'), may hold values from -0.09375 to 0.09375
- query_gain: float32 [64], replicated, may hold values from 0.4 to 9
- key_gain: float32 [64], replicated, may hold values from 0.4 to 9
- sinks: float32 [32], P('tp'), may hold values from 2 to 7
- w_mix: bfloat16 [8, 256, 256], P('tp'), may hold values from -0.375 to 0.375
- pool_scale: float32 [2048], P('tp'), may hold values from 0.1 to 1.9
- w_out_attn: bfloat16 [2048, 4096], P('sp', 'tp'), may hold values from -0.5 to 0.5
- w_out_pool: bfloat16 [2048, 4096], P('sp', 'tp'), may hold values from -0.125 to 0.125
Outputs:
- layer_out: bfloat16 [8192, 4096], P('sp', 'tp')
The draws below stay inside these ranges and needn't reach their ends.
All inputs are finite; a program needn't handle non-finite values.
Results may differ from the reference program's by a relative error of at most 0.0075.
The reference program's roundings to bfloat16 on the way count: a program that leaves them out, or rounds other values in their place, can miss the bound.
Values may be sent and summed in bfloat16 or wider, within the bound.
A program may use at most 128 MiB of HBM per device.

```python
import jax
import jax.numpy as jnp
from jax import lax

D = 4096
HEAD = 64
QHEADS = 32
KVHEADS = 8
POOL_GROUPS = 8
GROUP_DIM = 256
WINDOW = 128
TOKENS = 8192
ATTN_W = 2048
KV_W = 512
POOL_W = 2048


def draw_query_gain(key, part):
    subkey = jax.random.fold_in(key, 7)
    return jax.random.uniform(subkey, (HEAD,), jnp.float32, 0.4, 1.6)


def draw_key_gain(key, part):
    subkey = jax.random.fold_in(key, 11)
    return jax.random.uniform(subkey, (HEAD,), jnp.float32, 0.4, 1.6)


def level_of(stream_key, dims, split, low, high):
    loudness, own = 1.0, jax.random.fold_in(stream_key, 6)
    for dim, shards_of in split:
        steps = jnp.exp(jax.random.uniform(jax.random.fold_in(own, dim), (shards_of,), jnp.float32, low / len(split), high / len(split)))
        loudness = loudness * jnp.repeat(steps, dims[dim] // shards_of).reshape([-1 if axis == dim else 1 for axis in range(len(dims))])
    return loudness


def bell_draw(stream_key, shape, deviation, bound, split=(), kind=jnp.bfloat16):
    values = deviation * jax.random.normal(stream_key, shape, jnp.float32)
    if split:
        values = values * level_of(stream_key, shape, split, -0.22, 0.18)
    return jnp.clip(values, -bound, bound).astype(kind)


def setup_inputs(seed: int = 0) -> dict:
    seeds = jax.random.split(jax.random.key(seed), 14)
    tokens = bell_draw(seeds[0], (TOKENS, D), 1.0, 6.0, ((0, 16), (1, 2)))
    norm_gain = jnp.clip(1.0 + 0.18 * jax.random.normal(seeds[1], (D,), jnp.float32), 0.1, 1.9)
    w_query = bell_draw(seeds[2], (D, ATTN_W), D ** -0.5, 0.09375, ((0, 16), (1, 2)))
    w_key = bell_draw(seeds[3], (D, KV_W), D ** -0.5, 0.09375, ((0, 16), (1, 2)))
    w_value = bell_draw(seeds[4], (D, KV_W), D ** -0.5, 0.09375, ((0, 16), (1, 2)))
    w_pool_in = bell_draw(seeds[5], (D, POOL_W), D ** -0.5, 0.09375, ((0, 16), (1, 2)))
    query_gain = draw_query_gain(jax.random.fold_in(seeds[13], 71), 0)
    key_gain = draw_key_gain(jax.random.fold_in(seeds[13], 71), 0)
    sinks = jnp.clip(2.0 + 5.0 * jax.random.uniform(seeds[8], (QHEADS,), jnp.float32) ** level_of(seeds[8], (QHEADS,), ((0, 2),), -0.2, 0.2), 2.0, 7.0)
    w_mix = bell_draw(seeds[9], (POOL_GROUPS, GROUP_DIM, GROUP_DIM), GROUP_DIM ** -0.5, 0.375, ((0, 2),))
    pool_scale = jnp.clip(1.0 + 0.18 * jax.random.normal(seeds[10], (POOL_W,), jnp.float32), 0.1, 1.9)
    w_out_attn = bell_draw(seeds[11], (ATTN_W, D), (ATTN_W // 16) ** -0.5, 0.5, ((0, 16), (1, 2)))
    w_out_pool = bell_draw(seeds[12], (POOL_W, D), POOL_W ** -0.5, 0.125, ((0, 16), (1, 2)))
    return dict(tokens=tokens, norm_gain=norm_gain, w_query=w_query, w_key=w_key, w_value=w_value, w_pool_in=w_pool_in, query_gain=query_gain, key_gain=key_gain, sinks=sinks, w_mix=w_mix, pool_scale=pool_scale, w_out_attn=w_out_attn, w_out_pool=w_out_pool)


epsilon = 1e-06
longest_lag = 15

def row_norm(values, gain):
    return values * lax.rsqrt(lax.optimization_barrier(jnp.mean(values * values, axis=-1, keepdims=True)) + epsilon) * gain

def banded(source, blocks, padding):
    earlier = jnp.concatenate([padding, source[:-WINDOW]], axis=0).reshape(blocks, WINDOW, KVHEADS, HEAD)
    current = source.reshape(blocks, WINDOW, KVHEADS, HEAD)
    return jnp.concatenate([earlier, current], axis=1)

def reference(tokens, norm_gain, w_query, w_key, w_value, w_pool_in, query_gain, key_gain, sinks, w_mix, pool_scale, w_out_attn, w_out_pool):
    length = tokens.shape[0]
    normed = row_norm(tokens.astype(jnp.float32), norm_gain.astype(jnp.float32)).astype(jnp.bfloat16)
    queries = row_norm(jnp.dot(normed, w_query, preferred_element_type=jnp.float32).reshape(length, QHEADS, HEAD), query_gain.astype(jnp.float32)).astype(jnp.bfloat16)
    key_rows = row_norm(jnp.dot(normed, w_key, preferred_element_type=jnp.float32).reshape(length, KVHEADS, HEAD), key_gain.astype(jnp.float32)).astype(jnp.bfloat16)
    values = jnp.dot(normed, w_value, preferred_element_type=jnp.float32).astype(jnp.bfloat16).reshape(length, KVHEADS, HEAD)
    pool_in = jnp.dot(normed, w_pool_in, preferred_element_type=jnp.float32).astype(jnp.bfloat16)
    blocks = length // WINDOW
    per_kv = QHEADS // KVHEADS
    padding = jnp.zeros((WINDOW, KVHEADS, HEAD), jnp.bfloat16)
    band_keys = banded(key_rows, blocks, padding)
    band_values = banded(values, blocks, padding)
    query_blocks = queries.reshape(blocks, WINDOW, KVHEADS, per_kv, HEAD)
    query_index = jnp.arange(WINDOW)[:, None]
    key_index = jnp.arange(2 * WINDOW)[None, :]
    distance = query_index + WINDOW - key_index
    key_pos = jnp.arange(blocks)[:, None, None] * WINDOW - WINDOW + key_index[None]
    valid = (distance[None] >= 0) & (distance[None] < WINDOW) & (key_pos >= 0)
    sink_logit = sinks.astype(jnp.float32).reshape(KVHEADS, per_kv)

    def one_head(operands):
        head_queries, head_keys, head_values, head_sink = operands
        scores = jnp.einsum('bqgd,bjd->bgqj', head_queries.astype(jnp.float32), head_keys.astype(jnp.float32)) * HEAD ** (-0.5)
        scores = jnp.where(valid[:, None], scores, -1e+30)
        sink_col = head_sink[None, :, None, None]
        row_top = jnp.maximum(scores.max(axis=-1, keepdims=True), sink_col)
        lifted = jnp.exp(scores - row_top)
        weights = (lifted / (lifted.sum(axis=-1, keepdims=True) + jnp.exp(sink_col - row_top))).astype(jnp.bfloat16)
        return jnp.einsum('bgqj,bjd->bqgd', weights.astype(jnp.float32), head_values.astype(jnp.float32)).astype(jnp.bfloat16)
    head_out = lax.map(one_head, (jnp.moveaxis(query_blocks, 2, 0), jnp.moveaxis(band_keys, 2, 0), jnp.moveaxis(band_values, 2, 0), sink_logit))
    attended = jnp.transpose(head_out, (1, 2, 0, 3, 4)).reshape(length, ATTN_W)
    spans = 2 ** (1 + jnp.arange(POOL_W) // GROUP_DIM % 4)
    pool_wide = pool_in.astype(jnp.float32)
    extended = jnp.concatenate([jnp.zeros((longest_lag, POOL_W), jnp.float32), pool_wide], axis=0)
    window_sum = jnp.zeros((length, POOL_W), jnp.float32)
    for back_step in range(longest_lag + 1):
        shifted = extended[longest_lag - back_step:longest_lag - back_step + length]
        window_sum = window_sum + jnp.where(back_step < spans[None, :], shifted, 0.0)
    divisor = jnp.minimum(jnp.arange(1, length + 1).astype(jnp.float32)[:, None], spans.astype(jnp.float32)[None, :])
    contrast = (window_sum / divisor - pool_wide).astype(jnp.bfloat16)
    mixed = jnp.einsum('tgc,gcd->tgd', contrast.reshape(length, POOL_GROUPS, GROUP_DIM).astype(jnp.float32), w_mix.astype(jnp.float32)).reshape(length, POOL_W)
    pooled = (mixed * pool_scale.astype(jnp.float32)).astype(jnp.bfloat16)
    result = jnp.dot(attended, w_out_attn, preferred_element_type=jnp.float32) + jnp.dot(pooled, w_out_pool, preferred_element_type=jnp.float32)
    return result.astype(jnp.bfloat16)
```

```python
import jax
import jax.numpy as jnp
from jax import lax
from jax.sharding import Mesh
from jax.sharding import PartitionSpec as P

WINDOW = 128


epsilon = 1e-06
longest_lag = 15


def from_behind(block, axis):
    devices = range(lax.axis_size(axis))
    route = [(i - 1, i) for i in devices if i - 1 in devices]
    return lax.ppermute(block, axis, route)


def swap(block, axis):
    count = lax.axis_size(axis)
    return lax.ppermute(block, axis, [(i, count - 1 - i) for i in range(count)])


def row_norm(values, gain):
    return values * lax.rsqrt(jnp.mean(values * values, axis=-1, keepdims=True) + epsilon) * gain


def after(value, *others):
    return lax.optimization_barrier((value,) + others)[0]


def ordered(mine, theirs, index, dim):
    return jnp.where(
        index == 0,
        jnp.concatenate([mine, theirs], axis=dim),
        jnp.concatenate([theirs, mine], axis=dim),
    )


def both_cores(block, dim):
    if lax.axis_size("tp") == 2:
        return ordered(block, swap(block, "tp"), lax.axis_index("tp"), dim)
    return lax.all_gather(block, "tp", axis=dim, tiled=True)


def per_device(
    tokens,
    norm_gain,
    w_query,
    w_key,
    w_value,
    w_pool_in,
    query_gain,
    key_gain,
    sinks,
    w_mix,
    pool_scale,
    w_out_attn,
    w_out_pool,
):
    pair = lax.axis_size("si")
    place = lax.axis_index("si")
    outer = lax.axis_index("so")

    def share(array, owner, dim):
        size = array.shape[dim] // pair
        return lax.dynamic_slice_in_dim(array, owner * size, size, dim)

    def mine(arrays):
        return [share(a, place, 1) for a in arrays]

    def other(arrays):
        return [share(a, pair - 1 - place, 1) for a in arrays]

    def joined(own, came, dim):
        return own if pair == 1 else ordered(own, came, place, dim)

    def gathered(rows):
        return lax.all_gather(rows, "so", axis=0, tiled=True)

    qkv_parts = (w_query, w_key, w_value)
    qkv_own = jnp.concatenate(mine(qkv_parts), axis=1)
    if pair == 1:
        qkv_rows, pool_rows, attn_rows, mixed_rows = qkv_own, w_pool_in, w_out_attn, w_out_pool
        row_half = tokens
    else:
        qkv_came = swap(jnp.concatenate(other(qkv_parts), axis=1), "si")
        qkv_rows = joined(qkv_own, qkv_came, 0)
        late = lax.optimization_barrier((w_pool_in, w_out_attn, w_out_pool, qkv_came))[:3]
        came = [swap(share(w, pair - 1 - place, 1), "si") for w in late]
        pool_rows, attn_rows, mixed_rows = [
            joined(share(w, place, 1), c, 0) for w, c in zip((w_pool_in, w_out_attn, w_out_pool), came)
        ]
        row_half = joined(tokens, swap(after(tokens, qkv_came), "si"), 0)
    w_qkv = gathered(qkv_rows)
    w_pool = gathered(after(pool_rows, w_qkv))
    w_attn = gathered(after(attn_rows, w_pool))
    w_mixed = gathered(after(mixed_rows, w_attn))

    whole = both_cores(row_half, 1)
    row_count = whole.shape[0]
    normed = row_norm(whole.astype(jnp.float32), norm_gain).astype(jnp.bfloat16)
    qkv_raw = jnp.dot(normed, w_qkv, preferred_element_type=jnp.float32)
    head_size = query_gain.shape[0]
    query_width = w_query.shape[1] // pair
    kv_width = w_key.shape[1] // pair
    query_heads = query_width // head_size
    kv_local = kv_width // head_size
    per_kv = query_heads // kv_local
    query_raw = qkv_raw[:, :query_width]
    key_raw = qkv_raw[:, query_width : query_width + kv_width]
    value_raw = qkv_raw[:, query_width + kv_width :]
    queries = row_norm(query_raw.reshape(row_count, query_heads, head_size), query_gain).astype(
        jnp.bfloat16
    )
    key_rows = row_norm(key_raw.reshape(row_count, kv_local, head_size), key_gain).astype(
        jnp.bfloat16
    )
    values = value_raw.astype(jnp.bfloat16).reshape(row_count, kv_local, head_size)
    kv_tail = jnp.concatenate(
        [key_rows[-WINDOW:].reshape(WINDOW, -1), values[-WINDOW:].reshape(WINDOW, -1)], axis=1
    )
    kv_prev = from_behind(kv_tail, "so").reshape(WINDOW, 2, kv_local, head_size)
    offset = outer * row_count
    blocks = row_count // WINDOW

    def banded(previous, source):
        earlier = jnp.concatenate([previous, source[: row_count - WINDOW]], axis=0).reshape(
            blocks, WINDOW, kv_local, head_size
        )
        return jnp.concatenate(
            [earlier, source.reshape(blocks, WINDOW, kv_local, head_size)], axis=1
        )

    band_keys = banded(kv_prev[:, 0], key_rows)
    band_values = banded(kv_prev[:, 1], values)
    query_blocks = queries.reshape(blocks, WINDOW, kv_local, per_kv, head_size)
    scores = jnp.einsum(
        "bqkgd,bjkd->bkgqj", query_blocks, band_keys, preferred_element_type=jnp.float32
    ) * head_size ** (-0.5)
    query_index = jnp.arange(WINDOW)[:, None]
    key_index = jnp.arange(2 * WINDOW)[None, :]
    distance = query_index + WINDOW - key_index
    key_pos = offset + jnp.arange(blocks)[:, None, None] * WINDOW - WINDOW + key_index[None]
    valid = (distance[None] >= 0) & (distance[None] < WINDOW) & (key_pos >= 0)
    sink_logit = share(sinks, place, 0).reshape(kv_local, per_kv)[None, :, :, None, None]
    scores = jnp.where(valid[:, None, None], scores, -1e30)
    row_top = jnp.maximum(scores.max(axis=-1, keepdims=True), sink_logit)
    lifted = jnp.exp(scores - row_top)
    weights = (
        lifted / (lifted.sum(axis=-1, keepdims=True) + jnp.exp(sink_logit - row_top))
    ).astype(jnp.bfloat16)
    attended = (
        jnp.einsum("bkgqj,bjkd->bqkgd", weights, band_values, preferred_element_type=jnp.float32)
        .astype(jnp.bfloat16)
        .reshape(row_count, query_heads * head_size)
    )

    def all_heads(block):
        if pair == 2:
            block = joined(block, swap(block, "si"), 1)
        return both_cores(block, 1)

    attended_all = all_heads(attended)

    pool_in = jnp.dot(normed, w_pool, preferred_element_type=jnp.float32).astype(jnp.bfloat16)
    pool_prev = from_behind(pool_in[-longest_lag:], "so")
    mix = share(w_mix, place, 0)
    groups_local = mix.shape[0]
    group_dim = mix.shape[1]
    first_group = (lax.axis_index("tp") * pair + place) * groups_local
    group_ids = first_group + jnp.arange(groups_local, dtype=jnp.int32)
    spans = jnp.repeat(jnp.left_shift(jnp.int32(2), group_ids % 4), group_dim)
    extended = jnp.concatenate([pool_prev, pool_in], axis=0).astype(jnp.float32)
    window_sum = jnp.zeros((row_count, spans.shape[0]), jnp.float32)
    for back_step in range(longest_lag + 1):
        shifted = extended[longest_lag - back_step : longest_lag - back_step + row_count]
        window_sum = window_sum + jnp.where(back_step < spans[None, :], shifted, 0.0)
    positions = (offset + jnp.arange(1, row_count + 1, dtype=jnp.int32)).astype(jnp.float32)
    divisor = jnp.minimum(positions[:, None], spans.astype(jnp.float32)[None, :])
    contrast = (window_sum / divisor - extended[longest_lag:]).astype(jnp.bfloat16)
    mixed = jnp.einsum(
        "tgc,gcd->tgd",
        contrast.reshape(row_count, groups_local, group_dim),
        mix,
        preferred_element_type=jnp.float32,
    ).reshape(row_count, -1)
    pooled = (mixed * share(pool_scale, place, 0)).astype(jnp.bfloat16)
    pooled_all = all_heads(pooled)

    def project(owner):
        total = jnp.dot(share(attended_all, owner, 0), w_attn, preferred_element_type=jnp.float32)
        result = total + jnp.dot(
            share(pooled_all, owner, 0), w_mixed, preferred_element_type=jnp.float32
        )
        return result.astype(jnp.bfloat16)

    if pair == 1:
        return project(0)
    away = project(pair - 1 - place)
    came_back = swap(away, "si")
    return joined(project(place), came_back, 1)


def solution(mesh):
    sp, tp = mesh.shape["sp"], mesh.shape["tp"]

    def call(*args):
        kv_local = args[3].shape[1] // args[6].shape[0] // tp
        groups_local = args[9].shape[0] // tp
        fits = sp % 2 == 0 and kv_local % 2 == 0 and groups_local % 2 == 0
        pair = 2 if fits else 1
        inner = Mesh(mesh.devices.reshape(sp // pair, pair, tp), ("so", "si", "tp"))
        rows = ("so", "si")
        return jax.shard_map(
            per_device,
            mesh=inner,
            in_specs=(
                P(rows, "tp"),
                P(),
                P(rows, "tp"),
                P(rows, "tp"),
                P(rows, "tp"),
                P(rows, "tp"),
                P(),
                P(),
                P("tp"),
                P("tp", None, None),
                P("tp"),
                P(rows, "tp"),
                P(rows, "tp"),
            ),
            out_specs=P(rows, "tp"),
            check_vma=False,
        )(*args)

    return call
```
